32 devices in a mesh: fs: 4 (over y, x), tp: 8 (over z, core).
Axes of the slice: x: 2, y: 2, z: 4, core: 2. Of those that a mesh axis runs over, the one named last changes fastest.
Arguments:
- tokens: bfloat16 [4096, 2048], P(('fs', 'tp')), may hold values from -6 to 6
- up_weight: bfloat16 [2048, 4096], P('fs', 'tp'), may hold values from -0.125 to 0.125
- down_weight: bfloat16 [4096, 2048], P('tp', 'fs'), may hold values from -0.09375 to 0.09375
- cotangent: bfloat16 [4096, 2048], P(('fs', 'tp')), may hold values from -6 to 6
Outputs:
- input_grad: bfloat16 [4096, 2048], P(('fs', 'tp'))
- up_grad: float32 [2048, 4096], P('fs', 'tp')
- down_grad: float32 [4096, 2048], P('tp', 'fs')
The draws below stay inside these ranges and needn't reach their ends.
All inputs are finite; a program needn't handle non-finite values.
Results may differ from the reference program's by a relative error of at most 0.018.
Values may be sent and summed in bfloat16 or wider, within the bound.
A program may use at most 128 MiB of HBM per device.

```python
import jax
import jax.numpy as jnp
from jax import lax

D = 2048
FF = 4096
TOKENS = 4096
N_TP = 8


def spiked(entries, own_key, source, target, blocks, factor):
    owner, partner = [(jnp.arange(entries.shape[dim]) // (entries.shape[dim] // blocks)).reshape([-1 if axis == dim else 1 for axis in range(entries.ndim)]) for dim in (source, target)]
    chosen = jax.random.permutation(own_key, blocks)[partner]
    strong = (owner == chosen) | (owner == (partner + blocks // 2) % blocks)
    return jnp.where(strong, factor * entries, entries)


def levels(own_key, dims, pieces, low, high):
    loudness = 1.0
    for axis_at, parts in pieces:
        heights = jax.random.uniform(jax.random.fold_in(jax.random.fold_in(own_key, 6), axis_at), (parts,), jnp.float32, low / len(pieces), high / len(pieces))
        loudness = loudness * jnp.repeat(jnp.exp(heights), dims[axis_at] // parts).reshape((-1,) + (1,) * (len(dims) - 1 - axis_at))
    return loudness


def bell_draw(key, shape, spread, reach, split=(), kind=jnp.bfloat16):
    level = levels(key, shape, split, -0.22, 0.18) if split else 1.0
    drawn = jax.random.normal(key, shape, jnp.float32) * spread * level
    return jnp.minimum(jnp.maximum(drawn, -reach), reach).astype(kind)


def gaussian_with(rng, dims, spread, bound, pieces, heavy, held_as=jnp.bfloat16):
    values = spread * jax.random.normal(rng, dims, jnp.float32)
    if pieces:
        values = values * levels(rng, dims, pieces, -0.22, 0.18)
    return jnp.clip(spiked(values, jax.random.fold_in(rng, 3), *heavy), -bound, bound).astype(held_as)


def setup_inputs(seed: int = 0) -> dict:
    key_list = jax.random.split(jax.random.key(seed), 5)
    return {
        "tokens": bell_draw(key_list[0], (TOKENS, D), 1.0, 6.0, ((0, 32),)),
        "up_weight": bell_draw(key_list[1], (D, FF), D ** -0.5, 0.125, ((0, 4), (1, 8))),
        "down_weight": bell_draw(key_list[2], (FF, D), FF ** -0.5, 0.09375, ((0, 8), (1, 4))),
        "cotangent": gaussian_with(key_list[3], (TOKENS, D), 1.0, 6.0, ((0, 32),), (0, 1, 32, 2.75)),
    }


def reference(tokens, up_weight, down_weight, cotangent):
    pre = jnp.dot(tokens, up_weight, preferred_element_type=jnp.float32)
    active = jnp.maximum(pre, 0.0)
    hidden = (active * active).astype(jnp.bfloat16)
    dhidden = jnp.dot(cotangent, down_weight.T, preferred_element_type=jnp.float32)
    dpre = (2.0 * active * dhidden).astype(jnp.bfloat16)
    factor = 1.0 / jnp.sqrt(jnp.float32(TOKENS))
    down_grad = jnp.dot(hidden.T, cotangent, preferred_element_type=jnp.float32) * factor
    up_grad = jnp.dot(tokens.T, dpre, preferred_element_type=jnp.float32) * factor
    width = FF // N_TP

    def add_block(index, total):
        start = (index * width).astype(jnp.int32)
        cols = lax.dynamic_slice_in_dim(dpre, start, width, 1)
        right = lax.dynamic_slice_in_dim(up_weight, start, width, 1)
        part = jnp.dot(cols, right.T, preferred_element_type=jnp.float32).astype(jnp.bfloat16)
        part = lax.optimization_barrier(part)
        return total + part.astype(jnp.float32)
    total = lax.fori_loop(jnp.int32(0), jnp.int32(N_TP), add_block, jnp.zeros((TOKENS, D), jnp.float32))
    return (total.astype(jnp.bfloat16), up_grad, down_grad)
```

```python
import functools

import jax
import jax.numpy as jnp
from jax import lax
from jax.experimental import pallas as pl
from jax.experimental.pallas import tpu as pltpu
from jax.sharding import PartitionSpec as P

MESH = pl.DeviceIdType.MESH
BF16 = jnp.bfloat16
F32 = jnp.float32


def ring_index(p):
    q, b = p // 2, p % 2
    return 2 * q + b + (q % 2) * (1 - 2 * b)


def dot(a, b, ca, cb):
    return lax.dot_general(a, b, (((ca,), (cb,)), ((), ())), preferred_element_type=F32)


def kernel(
    nfs, nz, factor,
    tok_in, up_in, down_in, cot_in,
    dx_out, ug_out, dg_out,
    tok, cot, up, down, hid, dpre,
    dx_own, dx_send, dx_recv, dr_send, dr_recv,
    ug_own, dg_own, ug_send, ug_recv, dg_send, dg_recv,
    local_sem, zs, zr, ps, pr, ws, wr, gs, gr, xs, xr, rs, rr,
):
    fs, tp = lax.axis_index("fs"), lax.axis_index("tp")
    rows, width = tok_in.shape
    h = rows // 2
    block = 4 * h
    dl = up_in.shape[0]
    fl = up_in.shape[1]
    z, core = tp // 2, tp % 2
    pos = ring_index(fs)
    fwd = (fs, ((z + 1) % nz) * 2 + core)
    bwd = (fs, ((z + nz - 1) % nz) * 2 + core)
    mate = (fs, 2 * z + 1 - core)
    cw = (ring_index((pos + 1) % nfs), tp)
    ccw = (ring_index((pos + nfs - 1) % nfs), tp)

    def cols(o):
        return pl.ds(pl.multiple_of(o * dl, dl), dl)

    locals_ = [
        pltpu.make_async_copy(tok_in, tok.at[pl.ds(0, rows)], local_sem.at[0]),
        pltpu.make_async_copy(up_in, up.at[cols(fs)], local_sem.at[1]),
        pltpu.make_async_copy(down_in, down.at[:, cols(fs)], local_sem.at[2]),
        pltpu.make_async_copy(cot_in, cot.at[pl.ds(0, rows)], local_sem.at[3]),
    ]
    for c in locals_:
        c.start()
    barrier = pltpu.get_barrier_semaphore()
    peers = (fwd, bwd, mate, cw, ccw)
    for peer in peers:
        pl.semaphore_signal(barrier, inc=1, device_id=peer, device_id_type=MESH)
    pl.semaphore_wait(barrier, len(peers))
    for c in locals_:
        c.wait()

    sends = []

    def remote(src, dst, s, r, peer):
        c = pltpu.make_async_remote_copy(
            src_ref=src, dst_ref=dst, send_sem=s, recv_sem=r, device_id=peer, device_id_type=MESH
        )
        c.start()
        sends.append(c)
        return c

    bufs = (tok, cot)

    def z_send(k, a):
        out = []
        for d, peer in enumerate((fwd, bwd)):
            out.append(remote(
                bufs[a].at[pl.ds(k * block + d * h, h)],
                bufs[a].at[pl.ds((k + 1) * block + d * h, h)],
                zs.at[k, d, a], zr.at[k, d, a], peer,
            ))
        return out

    def mate_send(k, a):
        return remote(
            bufs[a].at[pl.ds(k * block, 2 * h)],
            bufs[a].at[pl.ds(k * block + 2 * h, 2 * h)],
            ps.at[k, a], pr.at[k, a], mate,
        )

    def w_send(k, half):
        a = ring_index((pos + nfs - k) % nfs)
        b = ring_index((pos + k) % nfs)
        n = dl // 2
        piece = up.at[pl.ds(pl.multiple_of(a * dl + half * n, n), n)]
        m = fl // 2
        other = down.at[pl.ds(half * m, m), cols(b)]
        return [
            remote(piece, piece, ws.at[k, half, 0], wr.at[k, half, 0], cw),
            remote(other, other, ws.at[k, half, 1], wr.at[k, half, 1], ccw),
        ]

    z_copy, w_copy, mate_copy = {}, {}, {}
    for a in range(2):
        z_copy[0, a] = z_send(0, a)
        w_copy[0, a] = w_send(0, a)
    for a in range(2):
        mate_copy[0, a] = mate_send(0, a)

    def hidden_block(s):
        here = pl.ds(s * block, block)
        active = jnp.maximum(dot(tok[here, :], up[...], 1, 0), 0.0)
        hid[here, :] = (active * active).astype(BF16)
        dh = dot(cot[here, :], down[...], 1, 1)
        dpre[here, :] = (2.0 * active * dh).astype(BF16)

    pair_copy = {}

    def dx_block(s):
        here = pl.ds(s * block, block)

        def tile(j, carry):
            c = cols(j)
            part = dot(dpre[here, :], up[c, :], 1, 1)
            dx_own[s, :, c] = part[: 2 * h]
            dx_send[s, :, c] = part[2 * h :].astype(BF16)
            return carry

        lax.fori_loop(0, nfs, tile, 0)
        pair_copy[s] = remote(dx_send.at[s], dx_recv.at[s], xs.at[s], xr.at[s], mate)

    events = []
    for k in range(nfs - 1):
        for half in range(2):
            events.append(((2 * k + half + 1) * 1.5 / (nfs - 1), 1, k, half))
    for k in range(nz - 1):
        for a in range(2):
            events.append(((2 * k + a + 1) * 3.0 / (nz - 1), 0, k, a))
    events.sort()
    weights_left = 2 * (nfs - 1)
    ready = [0]

    def settle(s):
        for a in range(2):
            mate_copy[s, a].wait_recv()
        hidden_block(s)
        if s < nz - 1:
            dx_block(s)

    for _, kind, k, a in events:
        if kind == 1:
            for c in w_copy[k, a]:
                c.wait_recv()
            if k + 1 < nfs - 1:
                w_copy[k + 1, a] = w_send(k + 1, a)
            weights_left -= 1
        else:
            for c in z_copy[k, a]:
                c.wait_recv()
            if k + 1 < nz - 1:
                z_copy[k + 1, a] = z_send(k + 1, a)
            mate_copy[k + 1, a] = mate_send(k + 1, a)
            if a == 1:
                ready.append(k + 1)
        if weights_left == 0:
            for s in ready:
                settle(s)
            ready = []
    for s in ready:
        settle(s)

    def up_term(r):
        o = ring_index((pos + nfs - r - 1) % nfs)
        return dot(tok[:, cols(o)], dpre[...], 0, 0)

    def down_term(r):
        o = ring_index((pos + r + 1) % nfs)
        return dot(hid[...], cot[:, cols(o)], 0, 0)

    g_copy = {}

    def g_send(r, half):
        n, m = dl // 2, fl // 2
        a, b = pl.ds(half * n, n), pl.ds(half * m, m)
        g_copy[r, half] = [
            remote(ug_send.at[r, a], ug_recv.at[r, a], gs.at[r, half, 0], gr.at[r, half, 0], cw),
            remote(dg_send.at[r, b], dg_recv.at[r, b], gs.at[r, half, 1], gr.at[r, half, 1], ccw),
        ]

    def g_first():
        ug_send[0] = up_term(0).astype(BF16)
        dg_send[0] = down_term(0).astype(BF16)
        for half in range(2):
            g_send(0, half)
        ug_own[...] = up_term(1)
        dg_own[...] = down_term(1)

    def g_step(r):
        n, m = dl // 2, fl // 2
        for half in range(2):
            for c in g_copy[r - 1, half]:
                c.wait_recv()
            a, b = pl.ds(half * n, n), pl.ds(half * m, m)
            gu = ug_own[a, :] + ug_recv[r - 1, a, :].astype(F32)
            gd = dg_own[b, :] + dg_recv[r - 1, b, :].astype(F32)
            if r < nfs - 1:
                ug_send[r, a, :] = gu.astype(BF16)
                dg_send[r, b, :] = gd.astype(BF16)
                g_send(r, half)
            else:
                ug_out[a, :] = gu * factor
                dg_out[b, :] = gd * factor
        if r < nfs - 1:
            ug_own[...] = up_term(r + 1)
            dg_own[...] = down_term(r + 1)

    x_copy = {}

    def x_step(r):
        s = r + 1 if r < nz - 1 else 0
        pair_copy[s].wait_recv()
        for d, peer in enumerate((fwd, bwd)):
            here = pl.ds(d * h, h)
            if r > 0:
                x_copy[r - 1, d].wait_recv()
            total = dx_own[s, here, :] + dx_recv[s, here, :].astype(F32)
            if r > 0:
                total = total + dr_recv[r - 1, here, :].astype(F32)
            if r < nz - 1:
                dr_send[r, here, :] = total.astype(BF16)
                x_copy[r, d] = remote(
                    dr_send.at[r, here], dr_recv.at[r, here], rs.at[r, d], rr.at[r, d], peer
                )
            else:
                dx_out[here, :] = total.astype(BF16)

    g_first()
    x_step(0)
    dx_block(nz - 1)
    for r in range(1, max(nfs, nz)):
        if r < nfs:
            g_step(r)
        if r < nz:
            x_step(r)
    for c in sends:
        c.wait_send()


def shards(nfs, ntp, tokens, up_weight, down_weight, cotangent):
    rows, width = tokens.shape
    dl, fl = up_weight.shape
    nz = ntp // 2
    whole = rows * ntp
    factor = 1.0 / (whole * nfs) ** 0.5
    dma = pltpu.SemaphoreType.DMA
    any_space = pl.BlockSpec(memory_space=pl.ANY)
    vmem = pl.BlockSpec(memory_space=pltpu.VMEM)
    return pl.pallas_call(
        functools.partial(kernel, nfs, nz, factor),
        out_shape=(
            jax.ShapeDtypeStruct((rows, width), BF16),
            jax.ShapeDtypeStruct((dl, fl), F32),
            jax.ShapeDtypeStruct((fl, dl), F32),
        ),
        in_specs=[any_space] * 4,
        out_specs=(vmem, vmem, vmem),
        scratch_shapes=[
            pltpu.VMEM((whole, width), BF16),
            pltpu.VMEM((whole, width), BF16),
            pltpu.VMEM((width, fl), BF16),
            pltpu.VMEM((fl, width), BF16),
            pltpu.VMEM((whole, fl), BF16),
            pltpu.VMEM((whole, fl), BF16),
            pltpu.VMEM((nz, rows, width), F32),
            pltpu.VMEM((nz, rows, width), BF16),
            pltpu.VMEM((nz, rows, width), BF16),
            pltpu.VMEM((nz - 1, rows, width), BF16),
            pltpu.VMEM((nz - 1, rows, width), BF16),
            pltpu.VMEM((dl, fl), F32),
            pltpu.VMEM((fl, dl), F32),
            pltpu.VMEM((nfs - 1, dl, fl), BF16),
            pltpu.VMEM((nfs - 1, dl, fl), BF16),
            pltpu.VMEM((nfs - 1, fl, dl), BF16),
            pltpu.VMEM((nfs - 1, fl, dl), BF16),
            dma((4,)),
            dma((nz - 1, 2, 2)), dma((nz - 1, 2, 2)),
            dma((nz, 2)), dma((nz, 2)),
            dma((nfs - 1, 2, 2)), dma((nfs - 1, 2, 2)),
            dma((nfs - 1, 2, 2)), dma((nfs - 1, 2, 2)),
            dma((nz,)), dma((nz,)),
            dma((nz - 1, 2)), dma((nz - 1, 2)),
        ],
        compiler_params=pltpu.CompilerParams(
            collective_id=0, has_side_effects=True, vmem_limit_bytes=67_000_000
        ),
    )(tokens, up_weight, down_weight, cotangent)


def solution(mesh):
    placed = (P(("fs", "tp"), None), P("fs", "tp"), P("tp", "fs"), P(("fs", "tp"), None))
    return jax.shard_map(
        functools.partial(shards, mesh.shape["fs"], mesh.shape["tp"]),
        mesh=mesh,
        in_specs=placed,
        out_specs=(P(("fs", "tp"), None), P("fs", "tp"), P("tp", "fs")),
        check_vma=False,
    )
```

```python
import functools

import jax
import jax.numpy as jnp
from jax import lax
from jax.experimental import pallas as pl
from jax.experimental.pallas import tpu as pltpu
from jax.sharding import PartitionSpec as P

MESH = pl.DeviceIdType.MESH
BF16 = jnp.bfloat16
F32 = jnp.float32


def ring_index(p):
    q, b = p // 2, p % 2
    return 2 * q + b + (q % 2) * (1 - 2 * b)


def dot(a, b, ca, cb):
    return lax.dot_general(a, b, (((ca,), (cb,)), ((), ())), preferred_element_type=F32)


def kernel(
    nfs, nz, factor,
    tok_in, up_in, down_in, cot_in,
    dx_out, ug_out, dg_out,
    tok, cot, up, down, hid, dpre,
    dx_own, dx_send, dx_recv, dr_send, dr_recv,
    ug_own, dg_own, ug_send, ug_recv, dg_send, dg_recv,
    local_sem, zs, zr, ps, pr, ws, wr, gs, gr, xs, xr, rs, rr,
):
    fs, tp = lax.axis_index("fs"), lax.axis_index("tp")
    rows, width = tok_in.shape
    h = rows // 2
    block = 4 * h
    dl = up_in.shape[0]
    fl = up_in.shape[1]
    z, core = tp // 2, tp % 2
    pos = ring_index(fs)
    fwd = (fs, ((z + 1) % nz) * 2 + core)
    bwd = (fs, ((z + nz - 1) % nz) * 2 + core)
    mate = (fs, 2 * z + 1 - core)
    cw = (ring_index((pos + 1) % nfs), tp)
    ccw = (ring_index((pos + nfs - 1) % nfs), tp)

    def cols(o):
        return pl.ds(pl.multiple_of(o * dl, dl), dl)

    locals_ = [
        pltpu.make_async_copy(tok_in, tok.at[pl.ds(0, rows)], local_sem.at[0]),
        pltpu.make_async_copy(up_in, up.at[cols(fs)], local_sem.at[1]),
        pltpu.make_async_copy(down_in, down.at[:, cols(fs)], local_sem.at[2]),
        pltpu.make_async_copy(cot_in, cot.at[pl.ds(0, rows)], local_sem.at[3]),
    ]
    for c in locals_:
        c.start()
    barrier = pltpu.get_barrier_semaphore()
    peers = (fwd, bwd, mate, cw, ccw)
    for peer in peers:
        pl.semaphore_signal(barrier, inc=1, device_id=peer, device_id_type=MESH)
    pl.semaphore_wait(barrier, len(peers))
    for c in locals_:
        c.wait()

    sends = []

    def remote(src, dst, s, r, peer):
        c = pltpu.make_async_remote_copy(
            src_ref=src, dst_ref=dst, send_sem=s, recv_sem=r, device_id=peer, device_id_type=MESH
        )
        c.start()
        sends.append(c)
        return c

    bufs = (tok, cot)

    def z_send(k, a):
        out = []
        for d, peer in enumerate((fwd, bwd)):
            out.append(remote(
                bufs[a].at[pl.ds(k * block + d * h, h)],
                bufs[a].at[pl.ds((k + 1) * block + d * h, h)],
                zs.at[k, d, a], zr.at[k, d, a], peer,
            ))
        return out

    def mate_send(k, a):
        return remote(
            bufs[a].at[pl.ds(k * block, 2 * h)],
            bufs[a].at[pl.ds(k * block + 2 * h, 2 * h)],
            ps.at[k, a], pr.at[k, a], mate,
        )

    def w_send(k, half):
        a = ring_index((pos + nfs - k) % nfs)
        b = ring_index((pos + k) % nfs)
        n = dl // 2
        piece = up.at[pl.ds(pl.multiple_of(a * dl + half * n, n), n)]
        m = fl // 2
        other = down.at[pl.ds(half * m, m), cols(b)]
        return [
            remote(piece, piece, ws.at[k, half, 0], wr.at[k, half, 0], cw),
            remote(other, other, ws.at[k, half, 1], wr.at[k, half, 1], ccw),
        ]

    z_copy, w_copy, mate_copy = {}, {}, {}
    for a in range(2):
        z_copy[0, a] = z_send(0, a)
        w_copy[0, a] = w_send(0, a)
    for a in range(2):
        mate_copy[0, a] = mate_send(0, a)

    def hidden_block(s):
        here = pl.ds(s * block, block)
        active = jnp.maximum(dot(tok[here, :], up[...], 1, 0), 0.0)
        hid[here, :] = (active * active).astype(BF16)
        dh = dot(cot[here, :], down[...], 1, 1)
        dpre[here, :] = (2.0 * active * dh).astype(BF16)

    pair_copy = {}

    def dx_block(s):
        here = pl.ds(s * block, block)

        def tile(j, carry):
            c = cols(j)
            part = dot(dpre[here, :], up[c, :], 1, 1)
            dx_own[s, :, c] = part[: 2 * h]
            dx_send[s, :, c] = part[2 * h :].astype(BF16)
            return carry

        lax.fori_loop(0, nfs, tile, 0)
        pair_copy[s] = remote(dx_send.at[s], dx_recv.at[s], xs.at[s], xr.at[s], mate)

    x_copy = {}

    def x_step(r):
        s = r + 1 if r < nz - 1 else 0
        pair_copy[s].wait_recv()
        for d, peer in enumerate((fwd, bwd)):
            here = pl.ds(d * h, h)
            if r > 0:
                x_copy[r - 1, d].wait_recv()
            total = dx_own[s, here, :] + dx_recv[s, here, :].astype(F32)
            if r > 0:
                total = total + dr_recv[r - 1, here, :].astype(F32)
            if r < nz - 1:
                dr_send[r, here, :] = total.astype(BF16)
                x_copy[r, d] = remote(
                    dr_send.at[r, here], dr_recv.at[r, here], rs.at[r, d], rr.at[r, d], peer
                )
            else:
                dx_out[here, :] = total.astype(BF16)

    events = []
    for k in range(nfs - 1):
        for half in range(2):
            events.append(((2 * k + half + 1) * 1.5 / (nfs - 1), 1, k, half))
    for k in range(nz - 1):
        for a in range(2):
            events.append(((2 * k + a + 1) * 3.0 / (nz - 1), 0, k, a))
    events.sort()
    weights_left = 2 * (nfs - 1)
    ready = [0]

    def settle(s):
        for a in range(2):
            mate_copy[s, a].wait_recv()
        hidden_block(s)
        if s < nz - 1:
            dx_block(s)

    for _, kind, k, a in events:
        if kind == 1:
            for c in w_copy[k, a]:
                c.wait_recv()
            if k + 1 < nfs - 1:
                w_copy[k + 1, a] = w_send(k + 1, a)
            weights_left -= 1
        else:
            for c in z_copy[k, a]:
                c.wait_recv()
            if k + 1 < nz - 1:
                z_copy[k + 1, a] = z_send(k + 1, a)
            mate_copy[k + 1, a] = mate_send(k + 1, a)
            if a == 1:
                ready.append(k + 1)
        if weights_left == 0 and (kind, k) != (0, nz - 2):
            for s in ready:
                settle(s)
            ready = []
    for s in ready[:-1]:
        settle(s)
    x_step(0)
    settle(ready[-1])

    def up_term(r):
        o = ring_index((pos + nfs - r - 1) % nfs)
        return dot(tok[:, cols(o)], dpre[...], 0, 0)

    def down_term(r):
        o = ring_index((pos + r + 1) % nfs)
        return dot(hid[...], cot[:, cols(o)], 0, 0)

    g_copy = {}

    def g_send(r, half, which):
        n, m = dl // 2, fl // 2
        a, b = pl.ds(half * n, n), pl.ds(half * m, m)
        if which == 0:
            g_copy[r, half, 0] = remote(
                ug_send.at[r, a], ug_recv.at[r, a], gs.at[r, half, 0], gr.at[r, half, 0], cw
            )
        else:
            g_copy[r, half, 1] = remote(
                dg_send.at[r, b], dg_recv.at[r, b], gs.at[r, half, 1], gr.at[r, half, 1], ccw
            )

    def g_terms(r):
        ug_own[...] = up_term(r)
        dg_own[...] = down_term(r)

    def g_first():
        ug_send[0] = up_term(0).astype(BF16)
        for half in range(2):
            g_send(0, half, 0)
        dg_send[0] = down_term(0).astype(BF16)
        for half in range(2):
            g_send(0, half, 1)
        g_terms(1)

    def g_step(r, half):
        n, m = dl // 2, fl // 2
        a, b = pl.ds(half * n, n), pl.ds(half * m, m)
        g_copy[r - 1, half, 0].wait_recv()
        gu = ug_own[a, :] + ug_recv[r - 1, a, :].astype(F32)
        if r < nfs - 1:
            ug_send[r, a, :] = gu.astype(BF16)
            g_send(r, half, 0)
        else:
            ug_out[a, :] = gu * factor
        g_copy[r - 1, half, 1].wait_recv()
        gd = dg_own[b, :] + dg_recv[r - 1, b, :].astype(F32)
        if r < nfs - 1:
            dg_send[r, b, :] = gd.astype(BF16)
            g_send(r, half, 1)
        else:
            dg_out[b, :] = gd * factor

    g_first()
    dx_block(nz - 1)
    for r in range(1, max(nfs, nz)):
        if r < nfs:
            g_step(r, 0)
        if r < nz:
            x_step(r)
        if r < nfs:
            g_step(r, 1)
            if r < nfs - 1:
                g_terms(r + 1)
    for c in sends:
        c.wait_send()


def shards(nfs, ntp, tokens, up_weight, down_weight, cotangent):
    rows, width = tokens.shape
    dl, fl = up_weight.shape
    nz = ntp // 2
    whole = rows * ntp
    factor = 1.0 / (whole * nfs) ** 0.5
    dma = pltpu.SemaphoreType.DMA
    any_space = pl.BlockSpec(memory_space=pl.ANY)
    vmem = pl.BlockSpec(memory_space=pltpu.VMEM)
    return pl.pallas_call(
        functools.partial(kernel, nfs, nz, factor),
        out_shape=(
            jax.ShapeDtypeStruct((rows, width), BF16),
            jax.ShapeDtypeStruct((dl, fl), F32),
            jax.ShapeDtypeStruct((fl, dl), F32),
        ),
        in_specs=[any_space] * 4,
        out_specs=(vmem, vmem, vmem),
        scratch_shapes=[
            pltpu.VMEM((whole, width), BF16),
            pltpu.VMEM((whole, width), BF16),
            pltpu.VMEM((width, fl), BF16),
            pltpu.VMEM((fl, width), BF16),
            pltpu.VMEM((whole, fl), BF16),
            pltpu.VMEM((whole, fl), BF16),
            pltpu.VMEM((nz, rows, width), F32),
            pltpu.VMEM((nz, rows, width), BF16),
            pltpu.VMEM((nz, rows, width), BF16),
            pltpu.VMEM((nz - 1, rows, width), BF16),
            pltpu.VMEM((nz - 1, rows, width), BF16),
            pltpu.VMEM((dl, fl), F32),
            pltpu.VMEM((fl, dl), F32),
            pltpu.VMEM((nfs - 1, dl, fl), BF16),
            pltpu.VMEM((nfs - 1, dl, fl), BF16),
            pltpu.VMEM((nfs - 1, fl, dl), BF16),
            pltpu.VMEM((nfs - 1, fl, dl), BF16),
            dma((4,)),
            dma((nz - 1, 2, 2)), dma((nz - 1, 2, 2)),
            dma((nz, 2)), dma((nz, 2)),
            dma((nfs - 1, 2, 2)), dma((nfs - 1, 2, 2)),
            dma((nfs - 1, 2, 2)), dma((nfs - 1, 2, 2)),
            dma((nz,)), dma((nz,)),
            dma((nz - 1, 2)), dma((nz - 1, 2)),
        ],
        compiler_params=pltpu.CompilerParams(
            collective_id=0, has_side_effects=True, vmem_limit_bytes=67_000_000
        ),
    )(tokens, up_weight, down_weight, cotangent)


def solution(mesh):
    placed = (P(("fs", "tp"), None), P("fs", "tp"), P("tp", "fs"), P(("fs", "tp"), None))
    return jax.shard_map(
        functools.partial(shards, mesh.shape["fs"], mesh.shape["tp"]),
        mesh=mesh,
        in_specs=placed,
        out_specs=(P(("fs", "tp"), None), P("fs", "tp"), P("tp", "fs")),
        check_vma=False,
    )
```
